256 devices in a mesh: sp: 32 (over z, y), tp: 8 (over x, core).
Axes of the slice: x: 4, y: 4, z: 8, core: 2. Of those that a mesh axis runs over, the one named last changes fastest.
Arguments:
- tokens: bfloat16 [16384, 2048], P('sp', 'tp'), may hold values from -64 to 64
- conv_input: bfloat16 [2048, 1024], P(None, 'tp'), may hold values from -0.125 to 0.125
- conv_inner: bfloat16 [2048, 1024], P(None, 'tp'), may hold values from -0.125 to 0.125
- conv_outer: bfloat16 [2048, 1024], P(None, 'tp'), may hold values from -0.125 to 0.125
- conv_gate: bfloat16 [2048, 1024], P(None, 'tp'), may hold values from -0.125 to 0.125
- conv_taps: bfloat16 [3, 1024], P(None, 'tp'), may hold values from -3.5 to 3.5
- query_proj: bfloat16 [2048, 1536], P(None, 'tp'), may hold values from -8 to 8
- latent_proj: bfloat16 [2048, 256], replicated, may hold values from -1 to 1
- rope_proj: bfloat16 [2048, 32], replicated, may hold values from -0.125 to 0.125
- latent_gain: float32 [256], replicated, may hold values from 0.1 to 1.9
- key_up: bfloat16 [256, 1024], P(None, 'tp'), may hold values from -2 to 2
- value_up: bfloat16 [256, 1024], P(None, 'tp'), may hold values from -0.375 to 0.375
- attn_gate: bfloat16 [2048, 1024], P(None, 'tp'), may hold values from -0.125 to 0.125
- conv_down: bfloat16 [1024, 2048], P('tp'), may hold values from -0.1875 to 0.1875
- attn_down: bfloat16 [1024, 2048], P('tp'), may hold values from -0.75 to 0.75
Outputs:
- layer_out: bfloat16 [16384, 2048], P(('sp', 'tp'))
The draws below stay inside these ranges and needn't reach their ends.
All inputs are finite; a program needn't handle non-finite values.
Results may differ from the reference program's by a relative error of at most 0.014.
Values may be sent and summed in bfloat16 or wider, within the bound.
No kernel may reach another device: no remote copies, remote signals or barrier semaphores. Data moves between devices by JAX's collectives and lax.ppermute only.
A program may use at most 128 MiB of HBM per device.

```python
import math
import jax
import jax.numpy as jnp
from jax import lax

D = 2048
D_CONV = 1024
HEADS = 16
NOPE = 64
ROPE = 32
VDIM = 64
KV = 256
GRID_W = 64
SEQ = 16384
N_TP = 8


def weight_pair(key):
    down_part = jnp.clip(jax.random.normal(jax.random.fold_in(key, 101), (D, KV), jnp.float32), -6.0, 6.0) * D ** (-0.5)
    up_part = jnp.clip(jax.random.normal(jax.random.fold_in(key, 102), (KV, HEADS * NOPE), jnp.float32), -6.0, 6.0) * KV ** (-0.5)
    return (down_part, up_part)


def draw_latent_proj(key, part):
    return jnp.clip(weight_pair(key)[0], -1.0, 1.0).astype(jnp.bfloat16)


def draw_key_up(key, part):
    return jnp.clip(weight_pair(key)[1], -2.0, 2.0).astype(jnp.bfloat16)


def draw_tokens(key, part):
    column = jnp.arange(D, dtype=jnp.float32) / max(D - 1, 1)
    col_noise = jax.random.uniform(jax.random.fold_in(key, 201), (D,), jnp.float32)
    row_exp = jax.random.uniform(jax.random.fold_in(key, 202), (SEQ,), jnp.float32, -0.5, 0.5)
    base_draw = jnp.clip(jax.random.normal(jax.random.fold_in(key, 204), (SEQ, D), jnp.float32), -6.0, 6.0)
    col_exp = 0.5 * column + 0.5 * col_noise - 0.5
    scaling = (10.0 ** row_exp)[:, None] * (10.0 ** col_exp)[None, :]
    values = base_draw * scaling
    return jnp.clip(values, -64.0, 64.0).astype(jnp.bfloat16)


def draw_query_proj(key, part):
    spread = (6.0 / D) ** 0.5
    whole_draw = jnp.clip(jax.random.normal(jax.random.fold_in(key, 303), (D, HEADS, NOPE + ROPE), jnp.float32), -6.0, 6.0) * spread
    return jnp.clip(whole_draw, -8.0, 8.0).reshape(D, HEADS * (NOPE + ROPE)).astype(jnp.bfloat16)


def block_levels(rng, shape, cuts, low, high):
    gain = 1.0
    for axis_at, shards_of in cuts:
        draws = jax.random.uniform(jax.random.fold_in(jax.random.fold_in(rng, 6), axis_at), (shards_of,), jnp.float32, low / len(cuts), high / len(cuts))
        gain = gain * jnp.repeat(jnp.exp(draws), shape[axis_at] // shards_of).reshape((-1,) + (1,) * (len(shape) - 1 - axis_at))
    return gain


def bell_draw(key, shape, width, bound, split=(), kind=jnp.bfloat16):
    array = width * jax.random.normal(key, shape, jnp.float32)
    if split:
        array = array * block_levels(key, shape, split, -0.22, 0.18)
    return jnp.clip(array, -bound, bound).astype(kind)


def setup_inputs(seed: int = 0) -> dict:
    splits = jax.random.split(jax.random.key(seed), 16)
    return {
        "tokens": draw_tokens(jax.random.fold_in(splits[15], 71), 0),
        "conv_input": bell_draw(splits[1], (D, D_CONV), D ** -0.5, 0.125, ((1, 8),)),
        "conv_inner": bell_draw(splits[2], (D, D_CONV), D ** -0.5, 0.125, ((1, 8),)),
        "conv_outer": bell_draw(splits[3], (D, D_CONV), D ** -0.5, 0.125, ((1, 8),)),
        "conv_gate": bell_draw(splits[4], (D, D_CONV), D ** -0.5, 0.125, ((1, 8),)),
        "conv_taps": bell_draw(splits[5], (3, D_CONV), 3 ** -0.5, 3.5, ((1, 8),)),
        "query_proj": draw_query_proj(jax.random.fold_in(splits[15], 71), 0),
        "latent_proj": draw_latent_proj(jax.random.fold_in(splits[15], 71), 0),
        "rope_proj": bell_draw(splits[8], (D, ROPE), D ** -0.5, 0.125),
        "latent_gain": jnp.clip(1.0 + 0.18 * jax.random.normal(splits[9], (KV,), jnp.float32), 0.1, 1.9),
        "key_up": draw_key_up(jax.random.fold_in(splits[15], 71), 0),
        "value_up": bell_draw(splits[11], (KV, HEADS * VDIM), KV ** -0.5, 0.375, ((1, 8),)),
        "attn_gate": bell_draw(splits[12], (D, HEADS * VDIM), D ** -0.5, 0.125, ((1, 8),)),
        "conv_down": bell_draw(splits[13], (D_CONV, D), D_CONV ** -0.5, 0.1875, ((0, 8),)),
        "attn_down": bell_draw(splits[14], (HEADS * VDIM, D), (HEADS * VDIM // 16) ** -0.5, 0.75, ((0, 8),)),
    }


rms_eps = 1e-06
rope_theta = 10000.0

def rounded(values):
    return lax.optimization_barrier(values.astype(jnp.bfloat16))

def axial_tables(positions, rope_width, grid_width):
    quarter = rope_width // 4
    frequency = rope_theta ** (-jnp.arange(quarter, dtype=jnp.float32) * 2.0 / (rope_width // 2))
    grid_row = (positions // grid_width).astype(jnp.float32)
    grid_col = (positions % grid_width).astype(jnp.float32)
    row_angle = grid_row[:, None] * frequency[None, :]
    col_angle = grid_col[:, None] * frequency[None, :]
    return (jnp.cos(row_angle), jnp.sin(row_angle), jnp.cos(col_angle), jnp.sin(col_angle))

def turn_half(vector, cos_table, sin_table):
    half_width = vector.shape[-1] // 2
    leading = vector[..., :half_width]
    trailing = vector[..., half_width:]
    return jnp.concatenate([leading * cos_table - trailing * sin_table, trailing * cos_table + leading * sin_table], axis=-1)

def axial_turn(vector, tables):
    half_width = vector.shape[-1] // 2
    return jnp.concatenate([turn_half(vector[..., :half_width], tables[0], tables[1]), turn_half(vector[..., half_width:], tables[2], tables[3])], axis=-1)

def reference(tokens, conv_input, conv_inner, conv_outer, conv_gate, conv_taps, query_proj, latent_proj, rope_proj, latent_gain, key_up, value_up, attn_gate, conv_down, attn_down):
    seq_len = tokens.shape[0]
    widened = tokens.astype(jnp.float32)
    row_scale = lax.rsqrt(lax.optimization_barrier(jnp.mean(widened * widened, axis=1, keepdims=True)) + rms_eps)

    def project(matrix):
        return jnp.dot(tokens, matrix, preferred_element_type=jnp.float32) * row_scale
    value_in = rounded(project(conv_input)).astype(jnp.float32)
    inner_in = rounded(project(conv_inner)).astype(jnp.float32)
    outer_in = rounded(project(conv_outer)).astype(jnp.float32)
    gate_in = rounded(project(conv_gate)).astype(jnp.float32)
    conv_product = rounded(inner_in * value_in).astype(jnp.float32)
    padded = jnp.pad(conv_product, ((1, 1), (0, 0)))
    tap_weights = conv_taps.astype(jnp.float32)
    conv_mixed = padded[:-2] * tap_weights[0] + padded[1:-1] * tap_weights[1] + padded[2:] * tap_weights[2]
    conv_out = (jax.nn.silu(gate_in) * outer_in * conv_mixed).astype(jnp.bfloat16)
    positions = jnp.arange(seq_len, dtype=jnp.int32)
    tables = axial_tables(positions, ROPE, GRID_W)
    head_tables = tuple((grid_table[:, None, :] for grid_table in tables))
    queries = project(query_proj).reshape(seq_len, HEADS, NOPE + ROPE)
    query_nope = queries[..., :NOPE].astype(jnp.bfloat16)
    query_rope = axial_turn(queries[..., NOPE:], head_tables).astype(jnp.bfloat16)
    latent = project(latent_proj)
    latent = (latent * lax.rsqrt(lax.optimization_barrier(jnp.mean(latent * latent, axis=1, keepdims=True)) + rms_eps) * latent_gain).astype(jnp.bfloat16)
    key_rope = axial_turn(project(rope_proj), tables).astype(jnp.bfloat16)
    key_nope = jnp.dot(latent, key_up, preferred_element_type=jnp.float32).astype(jnp.bfloat16).reshape(seq_len, HEADS, NOPE)
    key_values = jnp.dot(latent, value_up, preferred_element_type=jnp.float32).astype(jnp.bfloat16).reshape(seq_len, HEADS, VDIM)
    gate_attn = rounded(project(attn_gate)).astype(jnp.float32)
    key_wide = key_nope.astype(jnp.float32)
    rope_wide = key_rope.astype(jnp.float32)
    value_wide = key_values.astype(jnp.float32)
    block_rows = math.gcd(seq_len, 256)
    score_scale = (NOPE + ROPE) ** (-0.5)

    def attend_block(block_pair):
        nope_block, rope_block = block_pair
        scores = jnp.einsum('qhd,khd->hqk', nope_block.astype(jnp.float32), key_wide)
        scores = (scores + jnp.einsum('qhd,kd->hqk', rope_block.astype(jnp.float32), rope_wide)) * score_scale
        row_top = lax.optimization_barrier(jnp.max(scores, axis=2, keepdims=True))
        weights = jnp.exp(scores - row_top)
        weight_total = lax.optimization_barrier(jnp.sum(weights, axis=2))
        narrow = rounded(weights).astype(jnp.float32)
        attended = jnp.einsum('hqk,khd->qhd', narrow, value_wide) / weight_total.T[:, :, None]
        return attended.reshape(attended.shape[0], HEADS * VDIM)
    attended = lax.map(attend_block, (query_nope.reshape(-1, block_rows, HEADS, NOPE), query_rope.reshape(-1, block_rows, HEADS, ROPE)))
    attended = attended.reshape(seq_len, HEADS * VDIM)
    attn_out = (jax.nn.silu(gate_attn) * attended).astype(jnp.bfloat16)
    conv_width = D_CONV // N_TP
    head_width = HEADS // N_TP * VDIM
    conv_groups = conv_out.reshape(seq_len, N_TP, conv_width).transpose(1, 0, 2)
    attn_groups = attn_out.reshape(seq_len, N_TP, head_width).transpose(1, 0, 2)
    conv_blocks = conv_down.reshape(N_TP, conv_width, conv_down.shape[1])
    attn_blocks = attn_down.reshape(N_TP, head_width, attn_down.shape[1])

    def add_group(running_sum, group_terms):
        conv_part, conv_matrix, attn_part, attn_matrix = group_terms
        partial_sum = jnp.dot(conv_part, conv_matrix, preferred_element_type=jnp.float32) + jnp.dot(attn_part, attn_matrix, preferred_element_type=jnp.float32)
        return (running_sum + rounded(partial_sum).astype(jnp.float32), None)
    zeroed = jnp.zeros((seq_len, conv_down.shape[1]), jnp.float32)
    summed = lax.scan(add_group, zeroed, (conv_groups, conv_blocks, attn_groups, attn_blocks))[0]
    return summed.astype(jnp.bfloat16)
```

```python
import functools
import math

import jax
import jax.numpy as jnp
from jax import lax
from jax.experimental import pallas as pl
from jax.experimental.pallas import tpu as pltpu
from jax.sharding import Mesh
from jax.sharding import PartitionSpec as P

NOPE = 64
ROPE = 32
VDIM = 64
GRID_W = 64
EPS = 1e-06
THETA = 10000.0
LOG2E = 1.4426950408889634
SCALE = LOG2E / math.sqrt(NOPE + ROPE)

F32 = jnp.float32
BF16 = jnp.bfloat16
HEADS = 4
ROWS = 256
VROWS = 80
SEND_ROWS = 272
VM = pltpu.VMEM


def vspec():
    return pl.BlockSpec(memory_space=VM)


def sspec():
    return pl.BlockSpec(memory_space=pltpu.SMEM)


def nt(a, b):
    return lax.dot_general(a, b, (((1,), (1,)), ((), ())), preferred_element_type=F32)


def mm(a, b):
    return jnp.dot(a, b, preferred_element_type=F32)


def row_scale_of(pieces):
    total = None
    for p in pieces:
        wide = p[...].astype(F32)
        s = jnp.sum(wide * wide, axis=1, keepdims=True)
        total = s if total is None else total + s
    return lax.rsqrt(total / 2048.0 + EPS)


def summed(pieces, idx, slabs):
    acc = None
    for i, p in enumerate(pieces):
        at = pl.ds(pl.multiple_of(idx[i] * 256, 256), 256)
        w = slabs(at)
        d = mm(p[...], w)
        acc = d if acc is None else acc + d
    return acc


def proj_a_kernel(idx, *refs):
    pieces = refs[:8]
    w, tab, cs, gain, q_out, k_out = refs[8:]
    scale = row_scale_of(pieces)
    for n in range(2):
        part = summed(pieces, idx, lambda at: w[at, n * 256 : (n + 1) * 256])
        if n == 0:
            q_out[0:256, :] = jnp.transpose(part * (scale * SCALE)).astype(BF16)
        else:
            turned = jnp.transpose(part[:, :128] * (scale * SCALE))
            cr, sr, cc, sc = (tab[8 * j : 8 * j + 8, :] for j in range(4))
            rows = []
            for h in range(HEADS):
                a, b, c, d = (turned[32 * h + 8 * j : 32 * h + 8 * j + 8, :] for j in range(4))
                rows += [a * cr - b * sr, b * cr + a * sr, c * cc - d * sc, d * cc + c * sc]
            q_out[256:384, :] = jnp.concatenate(rows, axis=0).astype(BF16)
            rope = part[:, 128:256] * scale
            kr = rope * cs[:, 0:128] + pltpu.roll(rope, 96, 1) * cs[:, 128:256]
            k_out[:, 256:384] = kr.astype(BF16)
    z = summed(pieces, idx, lambda at: w[at, 512:768]) * scale
    z = z * lax.rsqrt(jnp.mean(z * z, axis=1, keepdims=True) + EPS) * gain[...]
    k_out[:, 0:256] = z.astype(BF16)


def proj_a(pieces, idx, w, tab, cs, gain):
    return pl.pallas_call(
        proj_a_kernel,
        out_shape=(
            jax.ShapeDtypeStruct((384, ROWS), BF16),
            jax.ShapeDtypeStruct((ROWS, 384), BF16),
        ),
        in_specs=[sspec()] + [vspec()] * 12,
        out_specs=(vspec(), vspec()),
        name="proj_a",
        cost_estimate=pl.CostEstimate(
            flops=2 * 256 * 2048 * 768, bytes_accessed=5 << 20, transcendentals=0
        ),
    )(idx, *pieces, w, tab, cs, gain)


def silu(v):
    return v / (1.0 + jnp.exp(-v))


def proj_b_kernel(idx, *refs):
    pieces = refs[:8]
    ws = refs[8:18]
    cp_out, gl_out, sg_out = refs[18:]
    scale = row_scale_of(pieces)

    def project(j):
        own, sib = ws[2 * j], ws[2 * j + 1]
        acc = summed(
            pieces, idx, lambda at: jnp.concatenate([own[at, :], sib[at, :]], axis=1)
        )
        return (acc * scale).astype(BF16).astype(F32)

    cp_out[...] = (project(0) * project(1)).astype(BF16)
    outer = project(2)
    gl_out[...] = silu(project(3)) * outer
    sg_out[...] = silu(jnp.transpose(project(4)))


def proj_b(pieces, idx, ws):
    return pl.pallas_call(
        proj_b_kernel,
        out_shape=(
            jax.ShapeDtypeStruct((ROWS, 256), BF16),
            jax.ShapeDtypeStruct((ROWS, 256), F32),
            jax.ShapeDtypeStruct((256, ROWS), F32),
        ),
        in_specs=[sspec()] + [vspec()] * 18,
        out_specs=(vspec(),) * 3,
        name="proj_b",
        cost_estimate=pl.CostEstimate(
            flops=2 * 256 * 2048 * 1280, bytes_accessed=7 << 20, transcendentals=0
        ),
    )(idx, *pieces, *ws)


def attend_kernel(n_keys, first, last, *refs):
    count = n_keys // 256
    keys = refs[:count]
    q, kup, vup = refs[count : count + 3]
    at = count + 3
    if not first:
        m_in, acc_in = refs[at : at + 2]
        at += 2
    if last:
        out = refs[at]
        at += 1
    else:
        m_out, acc_out = refs[at : at + 2]
        at += 2
    k_s, v_s = refs[at : at + 2]

    @pl.when(pl.program_id(0) == 0)
    def _():
        for i in range(count):
            lat = keys[i][:, 0:256]
            rope = keys[i][:, 256:384]
            span = slice(256 * i, 256 * i + 256)
            nope = mm(lat, kup[...]).astype(BF16)
            for p in range(2):
                k_s[p, span, 0:128] = nope[:, 128 * p : 128 * p + 128]
                k_s[p, span, 128:256] = rope
            val = nt(vup[...], lat).astype(BF16)
            ones = jnp.ones((VROWS - VDIM, 256), BF16)
            for h in range(HEADS):
                v_s[h, 0:VDIM, span] = val[VDIM * h : VDIM * h + VDIM, :]
                v_s[h, VDIM:VROWS, span] = ones

    for h in range(HEADS):
        p, e = h // 2, h % 2
        qn = q[0, 64 * h : 64 * h + 64, :]
        qr = q[0, 256 + 32 * h : 256 + 32 * h + 32, :]
        z64 = jnp.zeros((64, ROWS), BF16)
        z96 = jnp.zeros((96, ROWS), BF16)
        qt = jnp.concatenate([qn, z64, qr, z96] if e == 0 else [z64, qn, qr, z96], axis=0)
        s = mm(k_s[p], qt)
        top = jnp.max(s, axis=0, keepdims=True)
        if not first:
            old = m_in[0, h, 0:1, :]
            top = jnp.maximum(top, old)
        pr = jnp.exp2(s - top).astype(BF16)
        got = mm(v_s[h], pr)
        if not first:
            got = got + acc_in[0, h] * jnp.exp2(old - top)
        if last:
            total = got[VDIM : VDIM + 1, :]
            out[0, VDIM * h : VDIM * h + VDIM, :] = (got[:VDIM] / total).astype(BF16)
            level = top + jnp.log2(total)
            hi = level.astype(BF16)
            rest = level - hi.astype(F32)
            mid = rest.astype(BF16)
            lo = (rest - mid.astype(F32)).astype(BF16)
            if h == 0:
                levels = []
            levels.append((hi.astype(F32), mid.astype(F32), lo.astype(F32)))
        else:
            m_out[0, h] = jnp.broadcast_to(top, (8, ROWS))
            acc_out[0, h] = got
    if last:
        pack = [levels[h][j] for j in range(3) for h in range(HEADS)]
        pack.append(jnp.zeros((4, ROWS), F32))
        out[0, 256:SEND_ROWS, :] = jnp.concatenate(pack, axis=0).astype(BF16)


def attend(keys, q, kup, vup, state, last):
    first = state is None
    n_keys = 256 * len(keys)
    n_src = q.shape[0]
    whole = lambda shape: pl.BlockSpec(shape, lambda i: (0,) * len(shape))
    per = lambda *shape: pl.BlockSpec((1, *shape), lambda i: (i,) + (0,) * len(shape))
    in_specs = [whole((ROWS, 384))] * len(keys)
    in_specs += [per(384, ROWS), whole((256, 256)), whole((256, 256))]
    args = [*keys, q, kup, vup]
    if not first:
        in_specs += [per(HEADS, 8, ROWS), per(HEADS, VROWS, ROWS)]
        args += list(state)
    if last:
        out_shape = jax.ShapeDtypeStruct((n_src, SEND_ROWS, ROWS), BF16)
        out_specs = per(SEND_ROWS, ROWS)
    else:
        out_shape = (
            jax.ShapeDtypeStruct((n_src, HEADS, 8, ROWS), F32),
            jax.ShapeDtypeStruct((n_src, HEADS, VROWS, ROWS), F32),
        )
        out_specs = (per(HEADS, 8, ROWS), per(HEADS, VROWS, ROWS))
    pairs = n_src * ROWS * n_keys * HEADS
    return pl.pallas_call(
        functools.partial(attend_kernel, n_keys, first, last),
        out_shape=out_shape,
        grid=(n_src,),
        in_specs=in_specs,
        out_specs=out_specs,
        scratch_shapes=[
            VM((2, n_keys, 256), BF16),
            VM((HEADS, VROWS, n_keys), BF16),
        ],
        name="attend",
        cost_estimate=pl.CostEstimate(
            flops=pairs * 640, bytes_accessed=4 << 20, transcendentals=pairs
        ),
    )(*args)


def out_kernel(o0, o1, o2, o3, sg, conv, cd0, cd1, ad0, ad1, out):
    parts = (o0, o1, o2, o3)
    levels = []
    for o in parts:
        raw = o[256:SEND_ROWS, :].astype(F32)
        levels.append(raw[0:4] + raw[4:8] + raw[8:12])
    top = functools.reduce(jnp.maximum, levels)
    shares = [jnp.exp2(v - top) for v in levels]
    total = functools.reduce(jnp.add, shares)
    shares = [v / total for v in shares]
    rows = []
    for h in range(HEADS):
        mix = None
        for o, share in zip(parts, shares):
            term = o[VDIM * h : VDIM * h + VDIM, :].astype(F32) * share[h : h + 1, :]
            mix = term if mix is None else mix + term
        rows.append(mix)
    attn = jnp.transpose(jnp.concatenate(rows, axis=0) * sg[...]).astype(BF16)
    c = conv[...]
    for n in range(8):
        cols = slice(256 * n, 256 * n + 256)
        acc = mm(attn[:, 0:128], ad0[:, cols]) + mm(attn[:, 128:256], ad1[:, cols])
        acc = acc + mm(c[:, 0:128], cd0[:, cols]) + mm(c[:, 128:256], cd1[:, cols])
        out[:, cols] = acc.astype(BF16)


def out_proj(parts, sg, conv, downs):
    return pl.pallas_call(
        out_kernel,
        out_shape=jax.ShapeDtypeStruct((ROWS, 2048), BF16),
        in_specs=[vspec()] * 10,
        out_specs=vspec(),
        name="out_proj",
        cost_estimate=pl.CostEstimate(
            flops=2 * 256 * 512 * 2048, bytes_accessed=4 << 20, transcendentals=0
        ),
    )(*parts, sg, conv, *downs)


def ring(n, step):
    return [(i, (i + step) % n) for i in range(n)]


def on_device(
    tokens,
    conv_input,
    conv_inner,
    conv_outer,
    conv_gate,
    conv_taps,
    query_proj,
    latent_proj,
    rope_proj,
    latent_gain,
    key_up,
    value_up,
    attn_gate,
    conv_down,
    attn_down,
):
    nz, ny, nx = (lax.axis_size(a) for a in ("z", "y", "x"))
    x, c = lax.axis_index("x"), lax.axis_index("c")
    span = lax.axis_index("z") * ny + lax.axis_index("y")
    swap = lambda v: lax.ppermute(v, "c", [(0, 1), (1, 0)])
    right = lambda v: lax.ppermute(v, "x", ring(nx, 1))
    left = lambda v: lax.ppermute(v, "x", ring(nx, -1))

    blocks = tokens.reshape(4, 2, 64, 256)
    mine = lax.dynamic_index_in_dim(blocks, c, 1, keepdims=False).reshape(ROWS, 256)
    theirs = lax.dynamic_index_in_dim(blocks, 1 - c, 1, keepdims=False).reshape(ROWS, 256)
    got = swap(theirs)
    um, dm = right(mine), left(mine)
    ug, dg = right(got), left(got)
    om, og = right(um), left(dg)
    pieces = (mine, got, um, ug, dm, dg, om, og)
    sources = jnp.stack([x, x, x - 1, x - 1, x + 1, x + 1, x + 2, x + 2])
    idx = (((sources + 2 * nx) % nx) * 2 + jnp.stack([c, 1 - c] * 4)).astype(jnp.int32)

    q_sib = swap(query_proj)
    kup_sib, vup_sib = swap(key_up), swap(value_up)
    wide = (conv_input, conv_inner, conv_outer, conv_gate, attn_gate)
    pairs = []
    for w in wide:
        pairs += [w, swap(w)]
    downs = (conv_down, swap(conv_down), attn_down, swap(attn_down))
    taps = jnp.concatenate([conv_taps, swap(conv_taps)], axis=1).astype(F32)

    heads = [w.reshape(2048, 2, NOPE + ROPE) for w in (query_proj, q_sib)]
    nope = [w[:, :, :NOPE].reshape(2048, 2 * NOPE) for w in heads]
    rope = [w[:, :, NOPE:].reshape(2048, 2 * ROPE) for w in heads]
    r = rope_proj
    rot = jnp.concatenate([-r[:, 8:16], r[:, 0:8], -r[:, 24:32], r[:, 16:24]], axis=1)
    w_a = jnp.concatenate(
        [*nope, *rope, r, rot, jnp.zeros((2048, 64), BF16), latent_proj], axis=1
    )
    kup = jnp.concatenate([key_up, kup_sib], axis=1)
    vup = jnp.concatenate([value_up, vup_sib], axis=1).T

    row = jnp.arange(ROWS, dtype=jnp.int32)
    grid_row = (span * 8 + 2 * (row // 64) + c).astype(F32)
    grid_col = (row % GRID_W).astype(F32)
    freq = THETA ** (-jnp.arange(8, dtype=F32) * 2.0 / 16)
    ra, ca = freq[:, None] * grid_row[None, :], freq[:, None] * grid_col[None, :]
    tab = jnp.concatenate([jnp.cos(ra), jnp.sin(ra), jnp.cos(ca), jnp.sin(ca)], axis=0)
    cr, sr, cc, sc = (tab[8 * j : 8 * j + 8].T for j in range(4))
    pad = jnp.zeros((ROWS, 96), F32)
    cs = jnp.concatenate([cr, cr, cc, cc, pad, sr, sr, sc, sc, pad], axis=1)

    q_own, k_own = proj_a(pieces, idx, w_a, tab, cs, latent_gain[None, :])

    qs = jnp.stack([q_own] + [lax.ppermute(q_own, "y", ring(ny, s)) for s in (1, 2, 3)])
    k_sib = swap(k_own)
    steps = [[k_own, k_sib]]
    up, down = k_own, k_own
    for s in range(nz // 2):
        arrived = []
        up = lax.ppermute(up, "z", ring(nz, 1))
        arrived.append(up)
        if s < nz // 2 - 1:
            down = lax.ppermute(down, "z", ring(nz, -1))
            arrived.append(down)
        steps.append(arrived + [swap(v) for v in arrived])

    cp, gl, sg = proj_b(pieces, idx, pairs)

    state = None
    for i, keys in enumerate(steps):
        state = attend(keys, qs, kup, vup, state, i == len(steps) - 1)
    parts = [state[0]] + [lax.ppermute(state[s], "y", ring(ny, -s)) for s in (1, 2, 3)]

    cp4 = cp.reshape(4, 64, 256)
    flip = lambda v: jnp.concatenate([v[:, 128:], v[:, :128]], axis=1)
    edges = flip(swap(jnp.concatenate([cp4[:, 0], cp4[:, 63]], axis=0)))
    sib_first, sib_last = edges[:4], edges[4:]
    n_span = nz * ny
    forth = [(2 * s + 1, 2 * s + 2) for s in range(n_span - 1)]
    back = [(2 * s + 2, 2 * s + 1) for s in range(n_span - 1)]
    edge = flip(jnp.where(c == 1, cp[ROWS - 1 :], cp[:1]))
    outer = lax.ppermute(edge, ("z", "y", "c"), forth + back)
    before = jnp.where(c == 1, sib_last, jnp.concatenate([outer, sib_last[:3]], axis=0))
    after = jnp.where(c == 1, jnp.concatenate([sib_first[1:], outer], axis=0), sib_first)
    prev = jnp.concatenate([before[:, None], cp4[:, :-1]], axis=1).astype(F32)
    later = jnp.concatenate([cp4[:, 1:], after[:, None]], axis=1).astype(F32)
    mixed = prev * taps[0] + cp4.astype(F32) * taps[1] + later * taps[2]
    conv_out = (gl * mixed.reshape(ROWS, 256)).astype(BF16)

    partial = out_proj(parts, sg, conv_out, downs).reshape(nx, 64, 2048)
    arrived = lax.all_to_all(partial, "x", split_axis=0, concat_axis=0, tiled=True)
    return arrived.astype(F32).sum(axis=0).astype(BF16)


def solution(mesh):
    grid = Mesh(mesh.devices.reshape(8, 4, 4, 2), ("z", "y", "x", "c"))
    sp, tp = ("z", "y"), ("x", "c")
    cols, rows = P(None, tp), P(tp, None)
    placed = (P(sp, tp), *[cols] * 6, P(), P(), P(), *[cols] * 3, rows, rows)
    return jax.shard_map(
        on_device,
        mesh=grid,
        in_specs=placed,
        out_specs=P((*sp, *tp), None),
        check_vma=False,
    )
```

```python
import functools
import math

import jax
import jax.numpy as jnp
from jax import lax
from jax.experimental import pallas as pl
from jax.experimental.pallas import tpu as pltpu
from jax.sharding import Mesh
from jax.sharding import PartitionSpec as P

NOPE = 64
ROPE = 32
VDIM = 64
GRID_W = 64
EPS = 1e-06
THETA = 10000.0
LOG2E = 1.4426950408889634
SCALE = LOG2E / math.sqrt(NOPE + ROPE)

F32 = jnp.float32
BF16 = jnp.bfloat16
HEADS = 4
ROWS = 256
VROWS = 80
SEND_ROWS = 272
VM = pltpu.VMEM


def vspec():
    return pl.BlockSpec(memory_space=VM)


def sspec():
    return pl.BlockSpec(memory_space=pltpu.SMEM)


def nt(a, b):
    return lax.dot_general(a, b, (((1,), (1,)), ((), ())), preferred_element_type=F32)


def mm(a, b):
    return jnp.dot(a, b, preferred_element_type=F32)


def row_scale_of(pieces):
    total = None
    for p in pieces:
        wide = p[...].astype(F32)
        s = jnp.sum(wide * wide, axis=1, keepdims=True)
        total = s if total is None else total + s
    return lax.rsqrt(total / 2048.0 + EPS)


def feature_blocks():
    x, c = lax.axis_index("x"), lax.axis_index("c")
    offsets = []
    for step in (0, 3, 1, 2):
        source = lax.rem(x + step, 4)
        for core in (c, 1 - c):
            offsets.append(pl.multiple_of((source * 2 + core) * 256, 256))
    return offsets


def summed(pieces, dot):
    acc = None
    for p, at in zip(pieces, feature_blocks()):
        d = dot(p[...], pl.ds(at, 256))
        acc = d if acc is None else acc + d
    return acc


def turned(v, tab):
    cr, sr, cc, sc = (tab[8 * j : 8 * j + 8, :] for j in range(4))
    a, b, c, d = (v[8 * j : 8 * j + 8, :] for j in range(4))
    return [a * cr - b * sr, b * cr + a * sr, c * cc - d * sc, d * cc + c * sc]


def proj_a_kernel(*refs):
    pieces = refs[:8]
    q0, q1, rope_w, lat_w, gain, tab, kup0, kup1, vup0, vup1 = refs[8:18]
    q_out, k_out, kup_out, vup_out = refs[18:]
    scale = row_scale_of(pieces)
    flat = jnp.transpose(jnp.broadcast_to(scale, (ROWS, 128)))[0:1, :]
    t = tab[...]
    for i, w in enumerate((q0, q1)):
        part = summed(pieces, lambda p, at: nt(w[:, at], p)) * (flat * SCALE)
        for e in range(2):
            h = 2 * i + e
            q_out[64 * h : 64 * h + 64, :] = part[96 * e : 96 * e + 64].astype(BF16)
            rows = jnp.concatenate(turned(part[96 * e + 64 : 96 * e + 96], t), axis=0)
            q_out[256 + 32 * h : 288 + 32 * h, :] = rows.astype(BF16)
    part = summed(pieces, lambda p, at: nt(rope_w[:, at], p)) * flat
    rows = jnp.concatenate(turned(part, t) + [jnp.zeros((96, ROWS), F32)], axis=0)
    k_out[:, 256:384] = jnp.transpose(rows).astype(BF16)
    z = summed(pieces, lambda p, at: mm(p, lat_w[at, :])) * scale
    z = z * lax.rsqrt(jnp.mean(z * z, axis=1, keepdims=True) + EPS) * gain[...]
    k_out[:, 0:256] = z.astype(BF16)
    kup_out[...] = jnp.concatenate([kup0[...], kup1[...]], axis=1)
    for i, w in enumerate((vup0, vup1)):
        vup_out[128 * i : 128 * i + 128, :] = jnp.transpose(w[...].astype(F32)).astype(BF16)


def proj_a(pieces, *rest):
    return pl.pallas_call(
        proj_a_kernel,
        out_shape=(
            jax.ShapeDtypeStruct((384, ROWS), BF16),
            jax.ShapeDtypeStruct((ROWS, 384), BF16),
            jax.ShapeDtypeStruct((256, 256), BF16),
            jax.ShapeDtypeStruct((256, 256), BF16),
        ),
        in_specs=[vspec()] * 18,
        out_specs=(vspec(),) * 4,
        name="proj_a",
        cost_estimate=pl.CostEstimate(
            flops=2 * 256 * 2048 * 768, bytes_accessed=5 << 20, transcendentals=0
        ),
    )(*pieces, *rest)


def silu(v):
    return v / (1.0 + jnp.exp(-v))


def flip(v):
    return jnp.concatenate([v[:, 128:256], v[:, 0:128]], axis=1)


def proj_b_kernel(*refs):
    pieces = refs[:8]
    ws = refs[8:18]
    cp_out, gl_out, sg_out, edge_out, outer_out = refs[18:]
    scale = row_scale_of(pieces)

    def project(j):
        own, sib = ws[2 * j], ws[2 * j + 1]
        acc = summed(
            pieces, lambda p, at: mm(p, jnp.concatenate([own[at, :], sib[at, :]], axis=1))
        )
        return (acc * scale).astype(BF16).astype(F32)

    cp = project(0) * project(1)
    cp_out[...] = cp.astype(BF16)
    firsts = [cp[64 * b : 64 * b + 1] for b in range(4)]
    lasts = [cp[64 * b + 63 : 64 * b + 64] for b in range(4)]
    edge_out[...] = flip(jnp.concatenate(firsts + lasts, axis=0)).astype(BF16)
    outer = jnp.where(lax.axis_index("c") == 1, lasts[3], firsts[0])
    outer_out[...] = jnp.broadcast_to(flip(outer), (8, 256)).astype(BF16)
    outer_in = project(2)
    gl_out[...] = silu(project(3)) * outer_in
    sg_out[...] = silu(jnp.transpose(project(4)))


def proj_b(pieces, ws):
    return pl.pallas_call(
        proj_b_kernel,
        out_shape=(
            jax.ShapeDtypeStruct((ROWS, 256), BF16),
            jax.ShapeDtypeStruct((ROWS, 256), F32),
            jax.ShapeDtypeStruct((256, ROWS), F32),
            jax.ShapeDtypeStruct((8, 256), BF16),
            jax.ShapeDtypeStruct((8, 256), BF16),
        ),
        in_specs=[vspec()] * 18,
        out_specs=(vspec(),) * 5,
        name="proj_b",
        cost_estimate=pl.CostEstimate(
            flops=2 * 256 * 2048 * 1280, bytes_accessed=7 << 20, transcendentals=0
        ),
    )(*pieces, *ws)


def conv_kernel(cp, gl, edges, outer, t0, t1, out):
    second = lax.axis_index("c") == 1
    taps = jnp.concatenate([t0[...].astype(F32), t1[...].astype(F32)], axis=1)
    near = edges[...].astype(F32)
    far = outer[0:1, :].astype(F32)
    row = lax.broadcasted_iota(jnp.int32, (64, 256), 0)
    for b in range(4):
        block = cp[64 * b : 64 * b + 64, :].astype(F32)
        last, first = near[4 + b : 5 + b], near[b : b + 1]
        before = jnp.where(second, last, far if b == 0 else near[3 + b : 4 + b])
        after = jnp.where(second, far if b == 3 else near[b + 1 : b + 2], first)
        prev = jnp.where(row == 0, before, pltpu.roll(block, 1, 0))
        later = jnp.where(row == 63, after, pltpu.roll(block, 63, 0))
        mixed = prev * taps[0:1] + block * taps[1:2] + later * taps[2:3]
        out[64 * b : 64 * b + 64, :] = (gl[64 * b : 64 * b + 64, :] * mixed).astype(BF16)


def conv_mix(cp, gl, edges, outer, t0, t1):
    return pl.pallas_call(
        conv_kernel,
        out_shape=jax.ShapeDtypeStruct((ROWS, 256), BF16),
        in_specs=[vspec()] * 6,
        out_specs=vspec(),
        name="conv_mix",
        cost_estimate=pl.CostEstimate(
            flops=1 << 20, bytes_accessed=1 << 19, transcendentals=0
        ),
    )(cp, gl, edges, outer, t0, t1)


WIDE = 512
CHUNK = 512


def attend_kernel(count, first, last, *refs):
    n_keys = 256 * count
    keys = refs[:count]
    qs = refs[count : count + 4]
    kup, vup = refs[count + 4 : count + 6]
    at = count + 6
    if not first:
        m_in, acc_in = refs[at : at + 2]
        at += 2
    if last:
        outs = refs[at : at + 4]
        at += 4
    else:
        m_out, acc_out = refs[at : at + 2]
        at += 2
    k_s, v_s, s_s, q_s = refs[at : at + 4]

    @pl.when(pl.program_id(0) == 0)
    def _():
        for i in range(count):
            lat = keys[i][:, 0:256]
            rope = keys[i][:, 256:384]
            span = slice(256 * i, 256 * i + 256)
            nope = mm(lat, kup[...]).astype(BF16)
            for p in range(2):
                k_s[p, span, 0:128] = nope[:, 128 * p : 128 * p + 128]
                k_s[p, span, 128:256] = rope
            val = nt(vup[...], lat).astype(BF16)
            ones = jnp.ones((VROWS - VDIM, 256), BF16)
            for h in range(HEADS):
                v_s[h, 0:VDIM, span] = val[VDIM * h : VDIM * h + VDIM, :]
                v_s[h, VDIM:VROWS, span] = ones

    for g in range(2):

        @pl.when(pl.program_id(0) == g)
        def _():
            q_s[...] = jnp.concatenate([qs[2 * g][...], qs[2 * g + 1][...]], axis=1)

    def query(h):
        qn = q_s[64 * h : 64 * h + 64, :]
        qr = q_s[256 + 32 * h : 256 + 32 * h + 32, :]
        z64 = jnp.zeros((64, WIDE), BF16)
        z96 = jnp.zeros((96, WIDE), BF16)
        return jnp.concatenate([qn, z64, qr, z96] if h % 2 == 0 else [z64, qn, qr, z96], axis=0)

    steps = n_keys // CHUNK
    halves = (slice(0, 256), slice(256, 512))
    tops, outputs, levels = {}, [], []
    for h in range(HEADS + 1):
        g = h - 1
        if h < HEADS:
            qt = query(h)
            high = None if first else jnp.concatenate([m_in[0, h], m_in[1, h]], axis=1)
        if h > 0:
            got = None
            top = tops[g][0:1]
        for k in range(steps):
            part = slice(CHUNK * k, CHUNK * k + CHUNK)
            if h < HEADS:
                s = mm(k_s[h // 2, part, :], qt)
                s_s[h % 2, part, :] = s
                peak = jnp.max(s.reshape(CHUNK // 8, 8, WIDE), axis=0)
                high = peak if high is None else jnp.maximum(high, peak)
            if h > 0:
                e = jnp.exp2(s_s[g % 2, part, :] - top).astype(BF16)
                d = mm(v_s[g, :, part], e)
                got = d if got is None else got + d
        if h > 0:
            if not first:
                old = jnp.concatenate([m_in[0, g, 0:1], m_in[1, g, 0:1]], axis=1)
                held = jnp.concatenate([acc_in[0, g], acc_in[1, g]], axis=1)
                got = got + held * jnp.exp2(old - top)
            if last:
                total = got[VDIM : VDIM + 1, :]
                outputs.append((got[:VDIM] / total).astype(BF16))
                level = top + jnp.log2(total)
                hi = level.astype(BF16).astype(F32)
                mid = (level - hi).astype(BF16).astype(F32)
                levels.append((hi, mid, level - hi - mid))
            else:
                for j in range(2):
                    m_out[j, g] = tops[g][:, halves[j]]
                    acc_out[j, g] = got[:, halves[j]]
        if h < HEADS:
            tops[h] = jnp.broadcast_to(jnp.max(high, axis=0, keepdims=True), (8, WIDE))
    if last:
        pack = [levels[h][j] for j in range(3) for h in range(HEADS)]
        pack = jnp.concatenate(pack + [jnp.zeros((4, WIDE), F32)], axis=0).astype(BF16)
        whole = jnp.concatenate(outputs + [pack], axis=0)
        for g in range(2):

            @pl.when(pl.program_id(0) == g)
            def _():
                for j in range(2):
                    outs[2 * g + j][...] = whole[:, halves[j]]


def attend(keys, qs, kup, vup, state, last):
    first = state is None
    n_keys = 256 * len(keys)
    whole = lambda *shape: pl.BlockSpec(shape, lambda i: (0,) * len(shape))
    per = lambda *shape: pl.BlockSpec((2, *shape), lambda i: (i,) + (0,) * len(shape))
    state_specs = (per(HEADS, 8, ROWS), per(HEADS, VROWS, ROWS))
    in_specs = [whole(ROWS, 384)] * len(keys) + [whole(384, ROWS)] * 4
    in_specs += [whole(256, 256)] * 2
    args = [*keys, *qs, kup, vup]
    if not first:
        in_specs += list(state_specs)
        args += list(state)
    if last:
        out_shape = (jax.ShapeDtypeStruct((SEND_ROWS, ROWS), BF16),) * 4
        out_specs = (whole(SEND_ROWS, ROWS),) * 4
    else:
        out_shape = (
            jax.ShapeDtypeStruct((4, HEADS, 8, ROWS), F32),
            jax.ShapeDtypeStruct((4, HEADS, VROWS, ROWS), F32),
        )
        out_specs = state_specs
    pairs = 4 * ROWS * n_keys * HEADS
    return pl.pallas_call(
        functools.partial(attend_kernel, len(keys), first, last),
        out_shape=out_shape,
        grid=(2,),
        in_specs=in_specs,
        out_specs=out_specs,
        scratch_shapes=[
            VM((2, n_keys, 256), BF16),
            VM((HEADS, VROWS, n_keys), BF16),
            VM((2, n_keys, WIDE), F32),
            VM((384, WIDE), BF16),
        ],
        name="attend",
        cost_estimate=pl.CostEstimate(
            flops=pairs * 640, bytes_accessed=4 << 20, transcendentals=pairs
        ),
    )(*args)


def out_kernel(o0, o1, o2, o3, sg, conv, cd0, cd1, ad0, ad1, out):
    parts = (o0, o1, o2, o3)
    levels = []
    for o in parts:
        raw = o[256:SEND_ROWS, :].astype(F32)
        levels.append(raw[0:4] + raw[4:8] + raw[8:12])
    top = functools.reduce(jnp.maximum, levels)
    shares = [jnp.exp2(v - top) for v in levels]
    total = functools.reduce(jnp.add, shares)
    shares = [v / total for v in shares]
    rows = []
    for h in range(HEADS):
        mix = None
        for o, share in zip(parts, shares):
            term = o[VDIM * h : VDIM * h + VDIM, :].astype(F32) * share[h : h + 1, :]
            mix = term if mix is None else mix + term
        rows.append(mix)
    attn = jnp.transpose(jnp.concatenate(rows, axis=0) * sg[...]).astype(BF16)
    c = conv[...]
    for n in range(8):
        cols = slice(256 * n, 256 * n + 256)
        acc = mm(attn[:, 0:128], ad0[:, cols]) + mm(attn[:, 128:256], ad1[:, cols])
        acc = acc + mm(c[:, 0:128], cd0[:, cols]) + mm(c[:, 128:256], cd1[:, cols])
        out[:, cols] = acc.astype(BF16)


def out_proj(parts, sg, conv, downs):
    return pl.pallas_call(
        out_kernel,
        out_shape=jax.ShapeDtypeStruct((ROWS, 2048), BF16),
        in_specs=[vspec()] * 10,
        out_specs=vspec(),
        name="out_proj",
        cost_estimate=pl.CostEstimate(
            flops=2 * 256 * 512 * 2048, bytes_accessed=4 << 20, transcendentals=0
        ),
    )(*parts, sg, conv, *downs)


def ring(n, step):
    return [(i, (i + step) % n) for i in range(n)]


def on_device(
    tokens,
    conv_input,
    conv_inner,
    conv_outer,
    conv_gate,
    conv_taps,
    query_proj,
    latent_proj,
    rope_proj,
    latent_gain,
    key_up,
    value_up,
    attn_gate,
    conv_down,
    attn_down,
):
    nz, ny, nx = (lax.axis_size(a) for a in ("z", "y", "x"))
    c = lax.axis_index("c")
    span = lax.axis_index("z") * ny + lax.axis_index("y")
    swap = lambda v: lax.ppermute(v, "c", [(0, 1), (1, 0)])
    right = lambda v: lax.ppermute(v, "x", ring(nx, 1))
    left = lambda v: lax.ppermute(v, "x", ring(nx, -1))

    blocks = tokens.reshape(4, 2, 64, 256)
    theirs = lax.dynamic_index_in_dim(blocks, 1 - c, 1, keepdims=False).reshape(ROWS, 256)
    got = swap(theirs)
    mine = lax.dynamic_index_in_dim(blocks, c, 1, keepdims=False).reshape(ROWS, 256)
    um, dm = right(mine), left(mine)
    ug, dg = right(got), left(got)
    om, og = right(um), left(dg)
    pieces = (mine, got, um, ug, dm, dg, om, og)

    q_t = query_proj.T
    q_sib = swap(q_t)
    ups = (key_up, swap(key_up), value_up, swap(value_up))
    pairs = []
    for w in (conv_input, conv_inner, conv_outer, conv_gate, attn_gate):
        pairs += [w, swap(w)]
    downs = (conv_down, swap(conv_down), attn_down, swap(attn_down))
    taps_sib = swap(conv_taps)

    row = jnp.arange(ROWS, dtype=jnp.int32)
    grid_row = (span * 8 + 2 * (row // 64) + c).astype(F32)
    grid_col = (row % GRID_W).astype(F32)
    freq = THETA ** (-jnp.arange(8, dtype=F32) * 2.0 / 16)
    angle = freq[None, :, None] * jnp.stack([grid_row, grid_col])[:, None, :]
    tab = jnp.stack([jnp.cos(angle), jnp.sin(angle)], axis=1).reshape(32, ROWS)

    q_own, k_own, kup, vup = proj_a(
        pieces, q_t, q_sib, rope_proj.T, latent_proj, latent_gain[None, :], tab, *ups
    )

    qs = [q_own] + [lax.ppermute(q_own, "y", ring(ny, s)) for s in (1, 2, 3)]
    steps = [[k_own, swap(k_own)]]
    up, down = k_own, k_own
    for s in range(nz // 2):
        arrived = []
        up = lax.ppermute(up, "z", ring(nz, 1))
        arrived.append(up)
        if s < nz // 2 - 1:
            down = lax.ppermute(down, "z", ring(nz, -1))
            arrived.append(down)
        steps.append(arrived + [swap(v) for v in arrived])
    steps = [steps[0] + steps[1], *steps[2:]]

    late = lax.optimization_barrier((*pieces, q_own))[:8]
    cp, gl, sg, edge, outer = proj_b(late, pairs)
    n_span = nz * ny
    forth = [(2 * s + 1, 2 * s + 2) for s in range(n_span - 1)]
    back = [(2 * s + 2, 2 * s + 1) for s in range(n_span - 1)]
    edge = swap(edge)
    outer = lax.ppermute(outer, ("z", "y", "c"), forth + back)

    state = None
    for i, keys in enumerate(steps):
        state = attend(keys, qs, kup, vup, state, i == len(steps) - 1)
    parts = [state[0]] + [lax.ppermute(state[s], "y", ring(ny, -s)) for s in (1, 2, 3)]

    held = lax.optimization_barrier((cp, state[0]))[0]
    conv_out = conv_mix(held, gl, edge, outer, conv_taps, taps_sib)

    partial = out_proj(parts, sg, conv_out, downs).reshape(nx, 64, 2048)
    arrived = lax.all_to_all(partial, "x", split_axis=0, concat_axis=0, tiled=True)
    return arrived.astype(F32).sum(axis=0).astype(BF16)


def solution(mesh):
    grid = Mesh(mesh.devices.reshape(8, 4, 4, 2), ("z", "y", "x", "c"))
    sp, tp = ("z", "y"), ("x", "c")
    cols, rows = P(None, tp), P(tp, None)
    placed = (P(sp, tp), *[cols] * 6, P(), P(), P(), *[cols] * 3, rows, rows)
    return jax.shard_map(
        on_device,
        mesh=grid,
        in_specs=placed,
        out_specs=P((*sp, *tp), None),
        check_vma=False,
    )
```

```python
import functools
import math

import jax
import jax.numpy as jnp
from jax import lax
from jax.experimental import pallas as pl
from jax.experimental.pallas import tpu as pltpu
from jax.sharding import Mesh
from jax.sharding import PartitionSpec as P

NOPE = 64
ROPE = 32
VDIM = 64
GRID_W = 64
EPS = 1e-06
THETA = 10000.0
LOG2E = 1.4426950408889634
SCALE = LOG2E / math.sqrt(NOPE + ROPE)

F32 = jnp.float32
BF16 = jnp.bfloat16
HEADS = 4
ROWS = 256
VROWS = 80
SEND_ROWS = 272
KROWS = 288
VM = pltpu.VMEM


def vspec():
    return pl.BlockSpec(memory_space=VM)


def sspec():
    return pl.BlockSpec(memory_space=pltpu.SMEM)


def nt(a, b):
    return lax.dot_general(a, b, (((1,), (1,)), ((), ())), preferred_element_type=F32)


def mm(a, b):
    return jnp.dot(a, b, preferred_element_type=F32)


def feature_blocks():
    x, c = lax.axis_index("x"), lax.axis_index("c")
    offsets = []
    for step in (0, 3, 1, 2):
        source = lax.rem(x + step, 4)
        for core in (c, 1 - c):
            offsets.append(pl.multiple_of((source * 2 + core) * 256, 256))
    return offsets


def turned(v, tab):
    cr, sr, cc, sc = (tab[8 * j : 8 * j + 8, :] for j in range(4))
    a, b, c, d = (v[8 * j : 8 * j + 8, :] for j in range(4))
    return [a * cr - b * sr, b * cr + a * sr, c * cc - d * sc, d * cc + c * sc]


def proj_a_kernel(*refs):
    pieces = refs[:8]
    q0, q1, rope_w, lat_w, gain, tab, kup0, vup0, sib = refs[8:17]
    q_out, k_out, kup_out, vup_out, x_out, scale_out = refs[17:]
    total = None
    for p, at in zip(pieces, feature_blocks()):
        block = p[...]
        x_out[:, pl.ds(at, 256)] = block
        wide = block.astype(F32)
        part = jnp.sum(wide * wide, axis=1, keepdims=True)
        total = part if total is None else total + part
    scale = lax.rsqrt(total / 2048.0 + EPS)
    spread = jnp.broadcast_to(scale, (ROWS, 128))
    scale_out[...] = spread
    flat = jnp.transpose(spread)[0:1, :]
    t = tab[...]
    for i, w in enumerate((q0, q1)):
        part = nt(w[...], x_out[...]) * (flat * SCALE)
        for e in range(2):
            h = 2 * i + e
            q_out[64 * h : 64 * h + 64, :] = part[96 * e : 96 * e + 64].astype(BF16)
            rows = jnp.concatenate(turned(part[96 * e + 64 : 96 * e + 96], t), axis=0)
            q_out[256 + 32 * h : 288 + 32 * h, :] = rows.astype(BF16)
    part = nt(rope_w[...], x_out[...]) * flat
    k_out[256:KROWS, :] = jnp.concatenate(turned(part, t), axis=0).astype(BF16)
    z = mm(x_out[...], lat_w[...]) * scale
    z = z * lax.rsqrt(jnp.mean(z * z, axis=1, keepdims=True) + EPS) * gain[...]
    k_out[0:256, :] = z.astype(BF16)
    kup_out[...] = jnp.concatenate([kup0[...], sib[0:256, :]], axis=1)
    for i, w in enumerate((vup0[...], sib[256:512, :])):
        vup_out[128 * i : 128 * i + 128, :] = jnp.transpose(w.astype(F32)).astype(BF16)


def proj_a(pieces, *rest):
    return pl.pallas_call(
        proj_a_kernel,
        out_shape=(
            jax.ShapeDtypeStruct((384, ROWS), BF16),
            jax.ShapeDtypeStruct((KROWS, 256), BF16),
            jax.ShapeDtypeStruct((256, 256), BF16),
            jax.ShapeDtypeStruct((256, 256), BF16),
            jax.ShapeDtypeStruct((ROWS, 2048), BF16),
            jax.ShapeDtypeStruct((ROWS, 128), F32),
        ),
        in_specs=[vspec()] * 17,
        out_specs=(vspec(),) * 6,
        name="proj_a",
        cost_estimate=pl.CostEstimate(
            flops=2 * 256 * 2048 * 768, bytes_accessed=5 << 20, transcendentals=0
        ),
    )(*pieces, *rest)


def silu(v):
    return v / (1.0 + jnp.exp(-v))


def flip(v):
    return jnp.concatenate([v[:, 128:256], v[:, 0:128]], axis=1)


def proj_b_kernel(x, spread, *refs):
    ws, sib = refs[:5], refs[5:10]
    cp_out, gl_out, sg_out, edge_out, outer_out, w_s, r_s, sems = refs[10:]
    low, high = pl.ds(0, 128), pl.ds(128, 128)
    for j in range(5):
        pltpu.make_async_copy(ws[j], w_s.at[j, :, low], sems.at[0, j]).start()
        pltpu.make_async_copy(sib[j], w_s.at[j, :, high], sems.at[1, j]).start()
    scale = spread[:, 0:1]

    def one(j, carry):
        pltpu.make_async_copy(ws[0], w_s.at[j, :, low], sems.at[0, j]).wait()
        pltpu.make_async_copy(sib[0], w_s.at[j, :, high], sems.at[1, j]).wait()
        r_s[j] = mm(x[...], w_s[j]) * scale
        return carry

    lax.fori_loop(0, 5, one, 0)

    def project(j):
        return r_s[j].astype(BF16).astype(F32)

    cp = project(0) * project(1)
    cp_out[...] = cp.astype(BF16)
    firsts = [cp[64 * b : 64 * b + 1] for b in range(4)]
    lasts = [cp[64 * b + 63 : 64 * b + 64] for b in range(4)]
    edge_out[...] = flip(jnp.concatenate(firsts + lasts, axis=0)).astype(BF16)
    outer = jnp.where(lax.axis_index("c") == 1, lasts[3], firsts[0])
    outer_out[...] = jnp.broadcast_to(flip(outer), (8, 256)).astype(BF16)
    outer_in = project(2)
    gl_out[...] = silu(project(3)) * outer_in
    sg_out[...] = silu(jnp.transpose(project(4)))


def proj_b(x, spread, ws):
    return pl.pallas_call(
        proj_b_kernel,
        out_shape=(
            jax.ShapeDtypeStruct((ROWS, 256), BF16),
            jax.ShapeDtypeStruct((ROWS, 256), F32),
            jax.ShapeDtypeStruct((256, ROWS), F32),
            jax.ShapeDtypeStruct((8, 256), BF16),
            jax.ShapeDtypeStruct((8, 256), BF16),
        ),
        in_specs=[vspec()] * 2 + [pl.BlockSpec(memory_space=pl.ANY)] * 10,
        out_specs=(vspec(),) * 5,
        scratch_shapes=[
            VM((5, 2048, 256), BF16),
            VM((5, 256, 256), F32),
            pltpu.SemaphoreType.DMA((2, 5)),
        ],
        name="proj_b",
        cost_estimate=pl.CostEstimate(
            flops=2 * 256 * 2048 * 1280, bytes_accessed=7 << 20, transcendentals=0
        ),
    )(x, spread, *ws)


def conv_kernel(cp, gl, edges, outer, t0, t1, out):
    second = lax.axis_index("c") == 1
    t_sib = t1[512:528, :].astype(F32)[0:3]
    taps = jnp.concatenate([t0[...].astype(F32), t_sib], axis=1)
    near = edges[...].astype(F32)
    far = outer[0:1, :].astype(F32)
    row = lax.broadcasted_iota(jnp.int32, (64, 256), 0)
    for b in range(4):
        block = cp[64 * b : 64 * b + 64, :].astype(F32)
        last, first = near[4 + b : 5 + b], near[b : b + 1]
        before = jnp.where(second, last, far if b == 0 else near[3 + b : 4 + b])
        after = jnp.where(second, far if b == 3 else near[b + 1 : b + 2], first)
        prev = jnp.where(row == 0, before, pltpu.roll(block, 1, 0))
        later = jnp.where(row == 63, after, pltpu.roll(block, 63, 0))
        mixed = prev * taps[0:1] + block * taps[1:2] + later * taps[2:3]
        out[64 * b : 64 * b + 64, :] = (gl[64 * b : 64 * b + 64, :] * mixed).astype(BF16)


def conv_mix(cp, gl, edges, outer, t0, t1):
    return pl.pallas_call(
        conv_kernel,
        out_shape=jax.ShapeDtypeStruct((ROWS, 256), BF16),
        in_specs=[vspec()] * 6,
        out_specs=vspec(),
        name="conv_mix",
        cost_estimate=pl.CostEstimate(
            flops=1 << 20, bytes_accessed=1 << 19, transcendentals=0
        ),
    )(cp, gl, edges, outer, t0, t1)


WIDE = 512
SPAN = 512


def attend_kernel(count, first, last, *refs):
    keys = refs[:count]
    q0, q1, kup, vup = refs[count : count + 4]
    at = count + 4
    if not first:
        m_in, acc_in = refs[at : at + 2]
        at += 2
    outs = refs[at : at + 2]
    raw, k_s, v_s, s_s, q_s = refs[at + 2 : at + 7]
    m_s, acc_s = refs[at + 7 : at + 9] if last else outs

    for i in range(count):
        raw[i] = keys[i][...]
    if first:
        m_s[...] = jnp.full((HEADS, 8, WIDE), -jnp.inf, F32)
        acc_s[...] = jnp.zeros((HEADS, VROWS, WIDE), F32)
    else:
        m_s[...] = m_in[...]
        acc_s[...] = acc_in[...]
    for h in range(HEADS):
        v_s[h, VDIM:VROWS, :] = jnp.ones((VROWS - VDIM, SPAN), BF16)
        for j, q in enumerate((q0, q1)):
            cols = slice(256 * j, 256 * j + 256)
            lead = 64 * (h % 2)
            q_s[h, lead : lead + 64, cols] = q[64 * h : 64 * h + 64, :]
            q_s[h, 64 - lead : 128 - lead, cols] = jnp.zeros((64, 256), BF16)
            q_s[h, 128:160, cols] = q[256 + 32 * h : 288 + 32 * h, :]
            q_s[h, 160:256, cols] = jnp.zeros((96, 256), BF16)

    def one_span(i, carry):
        for t in range(2):
            lat = raw[i, t, 0:256, :]
            rope = raw[i, t, 256:KROWS, :].astype(F32)
            rope = jnp.transpose(jnp.concatenate([rope, jnp.zeros((96, 256), F32)], axis=0))
            span = slice(256 * t, 256 * t + 256)
            nope = mm(lat, kup[...]).astype(BF16)
            for p in range(2):
                k_s[p, span, 0:128] = nope[:, 128 * p : 128 * p + 128]
                k_s[p, span, 128:256] = rope.astype(BF16)
            val = nt(vup[...], lat).astype(BF16)
            for h in range(HEADS):
                v_s[h, 0:VDIM, span] = val[VDIM * h : VDIM * h + VDIM, :]
        tops = {}
        for h in range(HEADS + 1):
            g = h - 1
            if h < HEADS:
                s = mm(k_s[h // 2], q_s[h])
                s_s[h % 2] = s
                high = jnp.maximum(m_s[h], jnp.max(s.reshape(SPAN // 8, 8, WIDE), axis=0))
            if h > 0:
                top = tops[g][0:1]
                e = jnp.exp2(s_s[g % 2] - top).astype(BF16)
                shrink = jnp.exp2(m_s[g, 0:1] - top)
                acc_s[g] = acc_s[g] * shrink + mm(v_s[g], e)
                m_s[g] = tops[g]
            if h < HEADS:
                tops[h] = jnp.broadcast_to(jnp.max(high, axis=0, keepdims=True), (8, WIDE))
        return carry

    lax.fori_loop(0, count, one_span, 0)
    if last:
        levels = []
        for h in range(HEADS):
            total = acc_s[h, VDIM : VDIM + 1, :]
            done = (acc_s[h, 0:VDIM, :] / total).astype(BF16)
            level = m_s[h, 0:1, :] + jnp.log2(total)
            hi = level.astype(BF16).astype(F32)
            mid = (level - hi).astype(BF16).astype(F32)
            levels.append((hi, mid, level - hi - mid))
            for j in range(2):
                outs[j][VDIM * h : VDIM * h + VDIM, :] = done[:, 256 * j : 256 * j + 256]
        pack = [levels[h][j] for j in range(3) for h in range(HEADS)]
        pack = jnp.concatenate(pack + [jnp.zeros((4, WIDE), F32)], axis=0).astype(BF16)
        for j in range(2):
            outs[j][256:SEND_ROWS, :] = pack[:, 256 * j : 256 * j + 256]


def attend(keys, q0, q1, kup, vup, state, last):
    first = state is None
    count = len(keys)
    args = [*keys, q0, q1, kup, vup, *(() if first else state)]
    if last:
        out_shape = (jax.ShapeDtypeStruct((SEND_ROWS, ROWS), BF16),) * 2
    else:
        out_shape = (
            jax.ShapeDtypeStruct((HEADS, 8, WIDE), F32),
            jax.ShapeDtypeStruct((HEADS, VROWS, WIDE), F32),
        )
    scratch = [
        VM((count, 2, KROWS, 256), BF16),
        VM((2, SPAN, 256), BF16),
        VM((HEADS, VROWS, SPAN), BF16),
        VM((2, SPAN, WIDE), F32),
        VM((HEADS, 256, WIDE), BF16),
    ]
    if last:
        scratch += [VM((HEADS, 8, WIDE), F32), VM((HEADS, VROWS, WIDE), F32)]
    pairs = WIDE * SPAN * count * HEADS
    return pl.pallas_call(
        functools.partial(attend_kernel, count, first, last),
        out_shape=out_shape,
        in_specs=[vspec()] * len(args),
        out_specs=(vspec(),) * 2,
        scratch_shapes=scratch,
        name="attend",
        cost_estimate=pl.CostEstimate(
            flops=pairs * 640, bytes_accessed=3 << 20, transcendentals=pairs
        ),
    )(*args)


def out_kernel(o0, o1, sg, conv, cd0, ad0, sib, *refs):
    p2a, p2b, p1a, p1b, p3a, p3b, p0, lhs_s, rel_s, w_s, sems = refs
    copies = [
        pltpu.make_async_copy(w, w_s.at[pl.ds(128 * i, 128), :], sems.at[i])
        for i, w in enumerate((ad0, sib.at[1], cd0, sib.at[0]))
    ]
    for copy in copies:
        copy.start()
    levels = []
    for o in (o0, o1):
        raw = o[256:SEND_ROWS, :].astype(F32)
        levels.append(raw[0:4] + raw[4:8] + raw[8:12])
    top = jnp.maximum(*levels)
    shares = [jnp.exp2(v - top) for v in levels]
    total = shares[0] + shares[1]
    shares = [v / total for v in shares]
    rows = []
    for h in range(HEADS):
        part = slice(VDIM * h, VDIM * h + VDIM)
        rows.append(
            o0[part, :].astype(F32) * shares[0][h : h + 1]
            + o1[part, :].astype(F32) * shares[1][h : h + 1]
        )
    attn = jnp.transpose(jnp.concatenate(rows, axis=0) * sg[...]).astype(BF16)
    lhs_s[:, 0:256] = attn
    lhs_s[:, 256:512] = conv[...]
    x = lax.axis_index("x")
    for i in range(4):
        at = pl.multiple_of(lax.rem(x + i, 4) * 64, 64)
        rel_s[64 * i : 64 * i + 64, :] = lhs_s[pl.ds(at, 64), :]
    for copy in copies:
        copy.wait()
    for n in range(8):
        acc = mm(rel_s[...], w_s[:, 256 * n : 256 * n + 256]).astype(BF16)
        cols = slice(256 * (n % 4), 256 * (n % 4) + 256)
        p0[:, 256 * n : 256 * n + 256] = acc[0:64]
        (p1a if n < 4 else p1b)[:, cols] = acc[64:128]
        (p2a if n < 4 else p2b)[:, cols] = acc[128:192]
        (p3a if n < 4 else p3b)[:, cols] = acc[192:256]


def out_proj(o0, o1, sg, conv, downs):
    half = jax.ShapeDtypeStruct((64, 1024), BF16)
    return pl.pallas_call(
        out_kernel,
        out_shape=(half,) * 6 + (jax.ShapeDtypeStruct((64, 2048), BF16),),
        in_specs=[vspec()] * 4 + [pl.BlockSpec(memory_space=pl.ANY)] * 3,
        out_specs=(vspec(),) * 7,
        scratch_shapes=[
            VM((ROWS, 512), BF16),
            VM((ROWS, 512), BF16),
            VM((512, 2048), BF16),
            pltpu.SemaphoreType.DMA((4,)),
        ],
        name="out_proj",
        cost_estimate=pl.CostEstimate(
            flops=2 * 256 * 512 * 2048, bytes_accessed=4 << 20, transcendentals=0
        ),
    )(o0, o1, sg, conv, *downs)


def ring(n, step):
    return [(i, (i + step) % n) for i in range(n)]


def on_device(
    tokens,
    conv_input,
    conv_inner,
    conv_outer,
    conv_gate,
    conv_taps,
    query_proj,
    latent_proj,
    rope_proj,
    latent_gain,
    key_up,
    value_up,
    attn_gate,
    conv_down,
    attn_down,
):
    nz, ny, nx = (lax.axis_size(a) for a in ("z", "y", "x"))
    c = lax.axis_index("c")
    span = lax.axis_index("z") * ny + lax.axis_index("y")
    swap = lambda v: lax.ppermute(v, "c", [(0, 1), (1, 0)])
    right = lambda v: lax.ppermute(v, "x", ring(nx, 1))
    left = lambda v: lax.ppermute(v, "x", ring(nx, -1))

    blocks = tokens.reshape(4, 2, 64, 256)
    theirs = lax.dynamic_index_in_dim(blocks, 1 - c, 1, keepdims=False).reshape(ROWS, 256)
    got = swap(theirs)
    mine = lax.dynamic_index_in_dim(blocks, c, 1, keepdims=False).reshape(ROWS, 256)
    um, dm = right(mine), left(mine)
    ug, dg = right(got), left(got)
    om, og = right(um), left(dg)
    pieces = (mine, got, um, ug, dm, dg, om, og)

    q_t = query_proj.T
    q_sib = swap(q_t)
    wide_own = (conv_input, conv_inner, conv_outer, conv_gate, attn_gate)
    later = lax.optimization_barrier((conv_down, attn_down, um, dm, ug))
    pairs = (*wide_own, *[swap(w) for w in wide_own])
    small = jnp.concatenate([key_up, value_up, jnp.pad(conv_taps, ((0, 13), (0, 0)))], axis=0)
    small, downs = lax.optimization_barrier((small, jnp.stack(later[:2])))
    small_sib = swap(small)
    ups = (key_up, value_up, small_sib)
    downs = (conv_down, attn_down, swap(downs))

    row = jnp.arange(ROWS, dtype=jnp.int32)
    grid_row = (span * 8 + 2 * (row // 64) + c).astype(F32)
    grid_col = (row % GRID_W).astype(F32)
    freq = THETA ** (-jnp.arange(8, dtype=F32) * 2.0 / 16)
    angle = freq[None, :, None] * jnp.stack([grid_row, grid_col])[:, None, :]
    tab = jnp.stack([jnp.cos(angle), jnp.sin(angle)], axis=1).reshape(32, ROWS)

    q_own, k_own, kup, vup, x_all, spread = proj_a(
        pieces, q_t, q_sib, rope_proj.T, latent_proj, latent_gain[None, :], tab, *ups
    )

    q_pair = lambda v: lax.ppermute(v, "y", [(i, i ^ 1) for i in range(ny)])
    q_far = q_pair(q_own)
    k_far = lax.ppermute(k_own, "y", [(i, ny - 1 - i) for i in range(ny)])
    late = lax.optimization_barrier((x_all, spread, q_own))[:2]
    cp, gl, sg, edge, outer = proj_b(*late, pairs)

    k_far, q_far, _ = lax.optimization_barrier((k_far, q_far, cp))
    both = jnp.stack([k_own, k_far])

    n_span = nz * ny
    forth = [(2 * s + 1, 2 * s + 2) for s in range(n_span - 1)]
    back = [(2 * s + 2, 2 * s + 1) for s in range(n_span - 1)]
    near = (swap(edge), lax.ppermute(outer, ("z", "y", "c"), forth + back))

    send_up = lambda v: lax.ppermute(v, "z", ring(nz, 1))
    send_down = lambda v: lax.ppermute(v, "z", ring(nz, -1))
    score = lambda keys, state, last: attend(keys, q_own, q_far, kup, vup, state, last)
    coming = [send_up(both), send_down(both)]
    state = score([both, swap(both)], None, False)
    swapped = []
    for s in range(1, nz // 2 + 1):
        end = s == nz // 2
        held = lax.optimization_barrier((*coming, *near, state[0]))
        near, held = held[-3:-1], held[: len(coming)]
        if not end:
            coming = [send_up(held[0])]
            if s < nz // 2 - 1:
                coming.append(send_down(held[1]))
        crossing = [swap(v) for v in held]
        keys = [*held, *swapped, *(crossing if end else [])]
        state = score(keys, state, end)
        swapped = crossing
    o_far = q_pair(state[1])

    held = lax.optimization_barrier((cp, state[0]))[0]
    conv_out = conv_mix(held, gl, *near, conv_taps, small_sib)

    p2a, p2b, p1a, p1b, p3a, p3b, p0 = out_proj(state[0], o_far, sg, conv_out, downs)
    wide = lambda v: v.astype(F32)
    two_r, two_l = right(p2a), left(p2b)
    one_r, one_l = right(p1b), left(p3a)
    on_r = right((wide(p1a) + wide(two_r)).astype(BF16))
    on_l = left((wide(p3b) + wide(two_l)).astype(BF16))
    first = wide(p0[:, :1024]) + wide(on_r) + wide(one_l)
    second = wide(p0[:, 1024:]) + wide(on_l) + wide(one_r)
    return jnp.concatenate([first, second], axis=1).astype(BF16)


def solution(mesh):
    grid = Mesh(mesh.devices.reshape(8, 4, 4, 2), ("z", "y", "x", "c"))
    sp, tp = ("z", "y"), ("x", "c")
    cols, rows = P(None, tp), P(tp, None)
    placed = (P(sp, tp), *[cols] * 6, P(), P(), P(), *[cols] * 3, rows, rows)
    return jax.shard_map(
        on_device,
        mesh=grid,
        in_specs=placed,
        out_specs=P((*sp, *tp), None),
        check_vma=False,
    )
```

```python
import functools
import math

import jax
import jax.numpy as jnp
from jax import lax
from jax.experimental import pallas as pl
from jax.experimental.pallas import tpu as pltpu
from jax.sharding import Mesh
from jax.sharding import PartitionSpec as P

NOPE = 64
ROPE = 32
VDIM = 64
GRID_W = 64
EPS = 1e-06
THETA = 10000.0
LOG2E = 1.4426950408889634
SCALE = LOG2E / math.sqrt(NOPE + ROPE)

LIMIT = 20 * 2**20
F32 = jnp.float32
BF16 = jnp.bfloat16
HEADS = 4
ROWS = 256
VROWS = 80
SEND_ROWS = 272
KROWS = 288
VM = pltpu.VMEM
GRANT = pltpu.CompilerParams(vmem_limit_bytes=LIMIT)


def vspec():
    return pl.BlockSpec(memory_space=VM)


def sspec():
    return pl.BlockSpec(memory_space=pltpu.SMEM)


def nt(a, b):
    return lax.dot_general(a, b, (((1,), (1,)), ((), ())), preferred_element_type=F32)


def mm(a, b):
    return jnp.dot(a, b, preferred_element_type=F32)


def feature_blocks():
    x, c = lax.axis_index("x"), lax.axis_index("c")
    offsets = []
    for step in (0, 3, 1, 2):
        source = lax.rem(x + step, 4)
        for core in (c, 1 - c):
            offsets.append(pl.multiple_of((source * 2 + core) * 256, 256))
    return offsets


def turned(v, tab):
    cr, sr, cc, sc = (tab[8 * j : 8 * j + 8, :] for j in range(4))
    a, b, c, d = (v[8 * j : 8 * j + 8, :] for j in range(4))
    return [a * cr - b * sr, b * cr + a * sr, c * cc - d * sc, d * cc + c * sc]


def proj_a_kernel(*refs):
    pieces = refs[:8]
    q0, q1, rope_w, lat_w, gain, tab, kup0, vup0, sib = refs[8:17]
    q_out, k_out, kup_out, vup_out, x_out, scale_out = refs[17:]
    total = None
    for p, at in zip(pieces, feature_blocks()):
        block = p[...]
        x_out[:, pl.ds(at, 256)] = block
        wide = block.astype(F32)
        part = jnp.sum(wide * wide, axis=1, keepdims=True)
        total = part if total is None else total + part
    scale = lax.rsqrt(total / 2048.0 + EPS)
    spread = jnp.broadcast_to(scale, (ROWS, 128))
    scale_out[...] = spread
    flat = jnp.transpose(spread)[0:1, :]
    t = tab[...]
    for i, w in enumerate((q0, q1)):
        part = nt(w[...], x_out[...]) * (flat * SCALE)
        for e in range(2):
            h = 2 * i + e
            q_out[64 * h : 64 * h + 64, :] = part[96 * e : 96 * e + 64].astype(BF16)
            rows = jnp.concatenate(turned(part[96 * e + 64 : 96 * e + 96], t), axis=0)
            q_out[256 + 32 * h : 288 + 32 * h, :] = rows.astype(BF16)
    part = nt(rope_w[...], x_out[...]) * flat
    k_out[256:KROWS, :] = jnp.concatenate(turned(part, t), axis=0).astype(BF16)
    z = mm(x_out[...], lat_w[...]) * scale
    z = z * lax.rsqrt(jnp.mean(z * z, axis=1, keepdims=True) + EPS) * gain[...]
    k_out[0:256, :] = z.astype(BF16)
    kup_out[...] = jnp.concatenate([kup0[...], sib[0:256, :]], axis=1)
    for i, w in enumerate((vup0[...], sib[256:512, :])):
        vup_out[128 * i : 128 * i + 128, :] = jnp.transpose(w.astype(F32)).astype(BF16)


def proj_a(pieces, *rest):
    return pl.pallas_call(
        proj_a_kernel,
        out_shape=(
            jax.ShapeDtypeStruct((384, ROWS), BF16),
            jax.ShapeDtypeStruct((KROWS, 256), BF16),
            jax.ShapeDtypeStruct((256, 256), BF16),
            jax.ShapeDtypeStruct((256, 256), BF16),
            jax.ShapeDtypeStruct((ROWS, 2048), BF16),
            jax.ShapeDtypeStruct((ROWS, 128), F32),
        ),
        in_specs=[vspec()] * 17,
        out_specs=(vspec(),) * 6,
        name="proj_a",
        compiler_params=GRANT,
        cost_estimate=pl.CostEstimate(
            flops=2 * 256 * 2048 * 768, bytes_accessed=5 << 20, transcendentals=0
        ),
    )(*pieces, *rest)


def silu(v):
    return v / (1.0 + jnp.exp(-v))


def flip(v):
    return jnp.concatenate([v[:, 128:256], v[:, 0:128]], axis=1)


def proj_b_kernel(x, spread, *refs):
    ws, sib = refs[:5], refs[5:10]
    cp_out, gl_out, sg_out, edge_out, outer_out, w_s, r_s, sems = refs[10:]
    low, high = pl.ds(0, 128), pl.ds(128, 128)
    for j in range(5):
        pltpu.make_async_copy(ws[j], w_s.at[j, :, low], sems.at[0, j]).start()
        pltpu.make_async_copy(sib[j], w_s.at[j, :, high], sems.at[1, j]).start()
    scale = spread[:, 0:1]

    def one(j, carry):
        pltpu.make_async_copy(ws[0], w_s.at[j, :, low], sems.at[0, j]).wait()
        pltpu.make_async_copy(sib[0], w_s.at[j, :, high], sems.at[1, j]).wait()
        r_s[j] = mm(x[...], w_s[j]) * scale
        return carry

    lax.fori_loop(0, 5, one, 0)

    def project(j):
        return r_s[j].astype(BF16).astype(F32)

    cp = project(0) * project(1)
    cp_out[...] = cp.astype(BF16)
    firsts = [cp[64 * b : 64 * b + 1] for b in range(4)]
    lasts = [cp[64 * b + 63 : 64 * b + 64] for b in range(4)]
    edge_out[...] = flip(jnp.concatenate(firsts + lasts, axis=0)).astype(BF16)
    outer = jnp.where(lax.axis_index("c") == 1, lasts[3], firsts[0])
    outer_out[...] = jnp.broadcast_to(flip(outer), (8, 256)).astype(BF16)
    outer_in = project(2)
    gl_out[...] = silu(project(3)) * outer_in
    sg_out[...] = silu(jnp.transpose(project(4)))


def proj_b(x, spread, ws):
    return pl.pallas_call(
        proj_b_kernel,
        out_shape=(
            jax.ShapeDtypeStruct((ROWS, 256), BF16),
            jax.ShapeDtypeStruct((ROWS, 256), F32),
            jax.ShapeDtypeStruct((256, ROWS), F32),
            jax.ShapeDtypeStruct((8, 256), BF16),
            jax.ShapeDtypeStruct((8, 256), BF16),
        ),
        in_specs=[vspec()] * 2 + [pl.BlockSpec(memory_space=pl.ANY)] * 10,
        out_specs=(vspec(),) * 5,
        scratch_shapes=[
            VM((5, 2048, 256), BF16),
            VM((5, 256, 256), F32),
            pltpu.SemaphoreType.DMA((2, 5)),
        ],
        name="proj_b",
        compiler_params=GRANT,
        cost_estimate=pl.CostEstimate(
            flops=2 * 256 * 2048 * 1280, bytes_accessed=7 << 20, transcendentals=0
        ),
    )(x, spread, *ws)


def conv_kernel(cp, gl, edges, outer, t0, t1, out):
    second = lax.axis_index("c") == 1
    t_sib = t1[512:528, :].astype(F32)[0:3]
    taps = jnp.concatenate([t0[...].astype(F32), t_sib], axis=1)
    near = edges[...].astype(F32)
    far = outer[0:1, :].astype(F32)
    row = lax.broadcasted_iota(jnp.int32, (64, 256), 0)
    for b in range(4):
        block = cp[64 * b : 64 * b + 64, :].astype(F32)
        last, first = near[4 + b : 5 + b], near[b : b + 1]
        before = jnp.where(second, last, far if b == 0 else near[3 + b : 4 + b])
        after = jnp.where(second, far if b == 3 else near[b + 1 : b + 2], first)
        prev = jnp.where(row == 0, before, pltpu.roll(block, 1, 0))
        later = jnp.where(row == 63, after, pltpu.roll(block, 63, 0))
        mixed = prev * taps[0:1] + block * taps[1:2] + later * taps[2:3]
        out[64 * b : 64 * b + 64, :] = (gl[64 * b : 64 * b + 64, :] * mixed).astype(BF16)


def conv_mix(cp, gl, edges, outer, t0, t1):
    return pl.pallas_call(
        conv_kernel,
        out_shape=jax.ShapeDtypeStruct((ROWS, 256), BF16),
        in_specs=[vspec()] * 6,
        out_specs=vspec(),
        name="conv_mix",
        compiler_params=GRANT,
        cost_estimate=pl.CostEstimate(
            flops=1 << 20, bytes_accessed=1 << 19, transcendentals=0
        ),
    )(cp, gl, edges, outer, t0, t1)


WIDE = 512
SPAN = 512


def attend_kernel(given, count, first, last, *refs):
    keys = []
    for ref in refs[:given]:
        keys += [ref] if len(ref.shape) == 3 else [ref.at[0], ref.at[1]]
    kup, vup = refs[given : given + 2]
    at = given + 2
    if first:
        q0, q1 = refs[at : at + 2]
        outs, q_s = refs[at + 2 : at + 4], refs[at + 4]
        at += 5
    else:
        q_s, m_in, acc_in = refs[at : at + 3]
        outs = refs[at + 3 : at + 5]
        at += 5
    raw, k_s, v_s, s_s, sems = refs[at : at + 5]
    m_s, acc_s = refs[at + 5 : at + 7] if last else outs

    for i in range(count):
        pltpu.make_async_copy(keys[i], raw.at[i], sems.at[i]).start()
    if first:
        m_s[...] = jnp.full((HEADS, 8, WIDE), -jnp.inf, F32)
        acc_s[...] = jnp.zeros((HEADS, VROWS, WIDE), F32)
    else:
        m_s[...] = m_in[...]
        acc_s[...] = acc_in[...]
    for h in range(HEADS):
        v_s[h, VDIM:VROWS, :] = jnp.ones((VROWS - VDIM, SPAN), BF16)
        for j, q in enumerate((q0, q1) if first else ()):
            cols = slice(256 * j, 256 * j + 256)
            lead = 64 * (h % 2)
            q_s[h, lead : lead + 64, cols] = q[64 * h : 64 * h + 64, :]
            q_s[h, 64 - lead : 128 - lead, cols] = jnp.zeros((64, 256), BF16)
            q_s[h, 128:160, cols] = q[256 + 32 * h : 288 + 32 * h, :]
            q_s[h, 160:256, cols] = jnp.zeros((96, 256), BF16)

    def one_span(i, carry):
        pltpu.make_async_copy(keys[0], raw.at[i], sems.at[i]).wait()
        for t in range(2):
            lat = raw[i, t, 0:256, :]
            rope = raw[i, t, 256:KROWS, :].astype(F32)
            rope = jnp.transpose(jnp.concatenate([rope, jnp.zeros((96, 256), F32)], axis=0))
            span = slice(256 * t, 256 * t + 256)
            nope = mm(lat, kup[...]).astype(BF16)
            for p in range(2):
                k_s[p, span, 0:128] = nope[:, 128 * p : 128 * p + 128]
                k_s[p, span, 128:256] = rope.astype(BF16)
            val = nt(vup[...], lat).astype(BF16)
            for h in range(HEADS):
                v_s[h, 0:VDIM, span] = val[VDIM * h : VDIM * h + VDIM, :]
        tops = {}
        for h in range(HEADS + 1):
            g = h - 1
            if h < HEADS:
                s = mm(k_s[h // 2], q_s[h])
                s_s[h % 2] = s
                high = jnp.maximum(m_s[h], jnp.max(s.reshape(SPAN // 8, 8, WIDE), axis=0))
            if h > 0:
                top = tops[g][0:1]
                e = jnp.exp2(s_s[g % 2] - top).astype(BF16)
                shrink = jnp.exp2(m_s[g, 0:1] - top)
                acc_s[g] = acc_s[g] * shrink + mm(v_s[g], e)
                m_s[g] = tops[g]
            if h < HEADS:
                tops[h] = jnp.broadcast_to(jnp.max(high, axis=0, keepdims=True), (8, WIDE))
        return carry

    lax.fori_loop(0, count, one_span, 0)
    if last:
        levels = []
        for h in range(HEADS):
            total = acc_s[h, VDIM : VDIM + 1, :]
            done = (acc_s[h, 0:VDIM, :] / total).astype(BF16)
            level = m_s[h, 0:1, :] + jnp.log2(total)
            hi = level.astype(BF16).astype(F32)
            mid = (level - hi).astype(BF16).astype(F32)
            levels.append((hi, mid, level - hi - mid))
            for j in range(2):
                outs[j][VDIM * h : VDIM * h + VDIM, :] = done[:, 256 * j : 256 * j + 256]
        pack = [levels[h][j] for j in range(3) for h in range(HEADS)]
        pack = jnp.concatenate(pack + [jnp.zeros((4, WIDE), F32)], axis=0).astype(BF16)
        for j in range(2):
            outs[j][256:SEND_ROWS, :] = pack[:, 256 * j : 256 * j + 256]


def attend(keys, queries, kup, vup, state, last):
    first = state is None
    given = len(keys)
    count = sum(1 if k.ndim == 3 else 2 for k in keys)
    args = [*keys, kup, vup, *queries, *(() if first else state)]
    if last:
        out_shape = (jax.ShapeDtypeStruct((SEND_ROWS, ROWS), BF16),) * 2
    else:
        out_shape = (
            jax.ShapeDtypeStruct((HEADS, 8, WIDE), F32),
            jax.ShapeDtypeStruct((HEADS, VROWS, WIDE), F32),
        )
        if first:
            out_shape += (jax.ShapeDtypeStruct((HEADS, 256, WIDE), BF16),)
    scratch = [
        VM((count, 2, KROWS, 256), BF16),
        VM((2, SPAN, 256), BF16),
        VM((HEADS, VROWS, SPAN), BF16),
        VM((2, SPAN, WIDE), F32),
        pltpu.SemaphoreType.DMA((count,)),
    ]
    if last:
        scratch += [VM((HEADS, 8, WIDE), F32), VM((HEADS, VROWS, WIDE), F32)]
    pairs = WIDE * SPAN * count * HEADS
    return pl.pallas_call(
        functools.partial(attend_kernel, given, count, first, last),
        out_shape=out_shape,
        in_specs=[pl.BlockSpec(memory_space=pl.ANY)] * given + [vspec()] * (len(args) - given),
        out_specs=(vspec(),) * len(out_shape),
        scratch_shapes=scratch,
        name="attend",
        compiler_params=GRANT,
        cost_estimate=pl.CostEstimate(
            flops=pairs * 640, bytes_accessed=3 << 20, transcendentals=pairs
        ),
    )(*args)


def out_kernel(o0, o1, sg, conv, cd0, ad0, sib, *refs):
    p2a, p2b, p1, p3, p0, lhs_s, rel_s, w_s, sems = refs
    copies = [
        pltpu.make_async_copy(w, w_s.at[pl.ds(128 * i, 128), :], sems.at[i])
        for i, w in enumerate((ad0, sib.at[1], cd0, sib.at[0]))
    ]
    for copy in copies:
        copy.start()
    levels = []
    for o in (o0, o1):
        raw = o[256:SEND_ROWS, :].astype(F32)
        levels.append(raw[0:4] + raw[4:8] + raw[8:12])
    top = jnp.maximum(*levels)
    shares = [jnp.exp2(v - top) for v in levels]
    total = shares[0] + shares[1]
    shares = [v / total for v in shares]
    rows = []
    for h in range(HEADS):
        part = slice(VDIM * h, VDIM * h + VDIM)
        rows.append(
            o0[part, :].astype(F32) * shares[0][h : h + 1]
            + o1[part, :].astype(F32) * shares[1][h : h + 1]
        )
    attn = jnp.transpose(jnp.concatenate(rows, axis=0) * sg[...]).astype(BF16)
    lhs_s[:, 0:256] = attn
    lhs_s[:, 256:512] = conv[...]
    x = lax.axis_index("x")
    for i in range(4):
        at = pl.multiple_of(lax.rem(x + i, 4) * 64, 64)
        rel_s[64 * i : 64 * i + 64, :] = lhs_s[pl.ds(at, 64), :]
    for copy in copies:
        copy.wait()

    for side, far in ((0, p2a), (1, p2b)):

        def columns(n, carry):
            at = pl.multiple_of(n * 512, 512)
            cols = pl.ds(at + 1024 * side, 512)
            acc = mm(rel_s[...], w_s[:, cols]).astype(BF16)
            p0[:, cols] = acc[0:64]
            p1[:, cols] = acc[64:128]
            far[:, pl.ds(at, 512)] = acc[128:192]
            p3[:, cols] = acc[192:256]
            return carry

        lax.fori_loop(0, 2, columns, 0)


def out_proj(o0, o1, sg, conv, downs):
    half = jax.ShapeDtypeStruct((64, 1024), BF16)
    return pl.pallas_call(
        out_kernel,
        out_shape=(half,) * 2 + (jax.ShapeDtypeStruct((64, 2048), BF16),) * 3,
        in_specs=[vspec()] * 4 + [pl.BlockSpec(memory_space=pl.ANY)] * 3,
        out_specs=(vspec(),) * 5,
        scratch_shapes=[
            VM((ROWS, 512), BF16),
            VM((ROWS, 512), BF16),
            VM((512, 2048), BF16),
            pltpu.SemaphoreType.DMA((4,)),
        ],
        name="out_proj",
        compiler_params=GRANT,
        cost_estimate=pl.CostEstimate(
            flops=2 * 256 * 512 * 2048, bytes_accessed=4 << 20, transcendentals=0
        ),
    )(o0, o1, sg, conv, *downs)


def ring(n, step):
    return [(i, (i + step) % n) for i in range(n)]


def on_device(
    tokens,
    conv_input,
    conv_inner,
    conv_outer,
    conv_gate,
    conv_taps,
    query_proj,
    latent_proj,
    rope_proj,
    latent_gain,
    key_up,
    value_up,
    attn_gate,
    conv_down,
    attn_down,
):
    nz, ny, nx = (lax.axis_size(a) for a in ("z", "y", "x"))
    c = lax.axis_index("c")
    span = lax.axis_index("z") * ny + lax.axis_index("y")
    swap = lambda v: lax.ppermute(v, "c", [(0, 1), (1, 0)])
    right = lambda v: lax.ppermute(v, "x", ring(nx, 1))
    left = lambda v: lax.ppermute(v, "x", ring(nx, -1))

    blocks = tokens.reshape(4, 2, 64, 256)
    theirs = lax.dynamic_index_in_dim(blocks, 1 - c, 1, keepdims=False).reshape(ROWS, 256)
    got = swap(theirs)
    mine = lax.dynamic_index_in_dim(blocks, c, 1, keepdims=False).reshape(ROWS, 256)
    um, dm = right(mine), left(mine)
    ug, dg = right(got), left(got)
    om, og = right(um), left(dg)
    pieces = (mine, got, um, ug, dm, dg, om, og)

    q_t = query_proj.T
    q_sib = swap(q_t)
    wide_own = (conv_input, conv_inner, conv_outer, conv_gate, attn_gate)
    later = lax.optimization_barrier((conv_down, attn_down, um, dm, ug))
    pairs = (*wide_own, *[swap(w) for w in wide_own])
    small = jnp.concatenate([key_up, value_up, jnp.pad(conv_taps, ((0, 13), (0, 0)))], axis=0)
    small, downs = lax.optimization_barrier((small, jnp.stack(later[:2])))
    small_sib = swap(small)
    ups = (key_up, value_up, small_sib)
    downs = (conv_down, attn_down, swap(downs))

    row = jnp.arange(ROWS, dtype=jnp.int32)
    grid_row = (span * 8 + 2 * (row // 64) + c).astype(F32)
    grid_col = (row % GRID_W).astype(F32)
    freq = THETA ** (-jnp.arange(8, dtype=F32) * 2.0 / 16)
    angle = freq[None, :, None] * jnp.stack([grid_row, grid_col])[:, None, :]
    tab = jnp.stack([jnp.cos(angle), jnp.sin(angle)], axis=1).reshape(32, ROWS)

    q_own, k_own, kup, vup, x_all, spread = proj_a(
        pieces, q_t, q_sib, rope_proj.T, latent_proj, latent_gain[None, :], tab, *ups
    )

    q_pair = lambda v: lax.ppermute(v, "y", [(i, i ^ 1) for i in range(ny)])
    q_far = q_pair(q_own)
    k_far = lax.ppermute(k_own, "y", [(i, ny - 1 - i) for i in range(ny)])
    late = lax.optimization_barrier((x_all, spread, q_own))[:2]
    cp, gl, sg, edge, outer = proj_b(*late, pairs)

    k_far, q_far, _ = lax.optimization_barrier((k_far, q_far, cp))
    both = jnp.stack([k_own, k_far])

    n_span = nz * ny
    forth = [(2 * s + 1, 2 * s + 2) for s in range(n_span - 1)]
    back = [(2 * s + 2, 2 * s + 1) for s in range(n_span - 1)]
    near = (swap(edge), lax.ppermute(outer, ("z", "y", "c"), forth + back))

    send_up = lambda v: lax.ppermute(v, "z", ring(nz, 1))
    send_down = lambda v: lax.ppermute(v, "z", ring(nz, -1))
    coming = [send_up(both), send_down(both)]
    *state, queries = attend([both, swap(both)], (q_own, q_far), kup, vup, None, False)
    swapped = []
    for s in range(1, nz // 2 + 1):
        end = s == nz // 2
        held = lax.optimization_barrier((*coming, *near, state[0]))
        near, held = held[-3:-1], held[: len(coming)]
        if not end:
            coming = [send_up(held[0])]
            if s < nz // 2 - 1:
                coming.append(send_down(held[1]))
        crossing = [swap(held[0] if len(held) == 1 else jnp.stack(held))]
        keys = [*held, *swapped, *(crossing if end else [])]
        state = attend(keys, (queries,), kup, vup, state, end)
        swapped = crossing
    o_far = q_pair(state[1])

    held = lax.optimization_barrier((cp, state[0]))[0]
    conv_out = conv_mix(held, gl, *near, conv_taps, small_sib)

    p2a, p2b, p1, p3, p0 = out_proj(state[0], o_far, sg, conv_out, downs)
    wide = lambda v: v.astype(F32)
    join = lambda a, b: jnp.concatenate([a, b], axis=1)
    two_r, two_l = right(p2a), left(p2b)
    on_r = right(join((wide(p1[:, :1024]) + wide(two_r)).astype(BF16), p1[:, 1024:]))
    on_l = left(join(p3[:, :1024], (wide(p3[:, 1024:]) + wide(two_l)).astype(BF16)))
    return (wide(p0) + wide(on_r) + wide(on_l)).astype(BF16)


def solution(mesh):
    grid = Mesh(mesh.devices.reshape(8, 4, 4, 2), ("z", "y", "x", "c"))
    sp, tp = ("z", "y"), ("x", "c")
    cols, rows = P(None, tp), P(tp, None)
    placed = (P(sp, tp), *[cols] * 6, P(), P(), P(), *[cols] * 3, rows, rows)
    return jax.shard_map(
        on_device,
        mesh=grid,
        in_specs=placed,
        out_specs=P((*sp, *tp), None),
        check_vma=False,
    )
```
